256 devices in a mesh: sp: 32 (over z, y), tp: 8 (over x, core).
Axes of the slice: x: 4, y: 4, z: 8, core: 2. Of those that a mesh axis runs over, the one named last changes fastest.
Arguments:
- tokens: bfloat16 [16384, 2048], P(('sp', 'tp')), may hold values from -8 to 8, as said below
- w_query: bfloat16 [2048, 1024], P(None, 'tp'), may hold values from -0.125 to 0.125
- w_key: bfloat16 [2048, 1024], P(None, 'tp'), may hold values from -0.125 to 0.125
- w_value: bfloat16 [2048, 1024], P(None, 'tp'), may hold values from -0.125 to 0.125
- head_bias: float32 [16], P('tp'), may hold values from -40 to -3
- w_out: bfloat16 [1024, 2048], P('tp'), may hold values from -0.1875 to 0.1875
Outputs:
- mixed: bfloat16 [16384, 2048], P(('sp', 'tp'))
The draws below stay inside these ranges and needn't reach their ends.
Inputs may be any that keep to these rules, and one draw needn't show every extreme that they name: `tokens`: activations of order one whose mean shifts between blocks of 512 positions.
All inputs are finite; a program needn't handle non-finite values.
Results may differ from the reference program's by a relative error of at most 0.014.
Values may be sent and summed in bfloat16 or wider, within the bound.
No kernel may reach another device: no remote copies, remote signals or barrier semaphores. Data moves between devices by JAX's collectives and lax.ppermute only.
A program may use at most 128 MiB of HBM per device.

```python
import jax
import jax.numpy as jnp
from jax import lax

D = 2048
HEADS = 16
HEAD_DIM = 64
TOK_DEV = 512
TOKENS = 16384
N_SP = 32
N_TP = 8


def draw_tokens(key, part):
    noise = jax.random.normal(jax.random.fold_in(key, 11), (TOKENS, D), jnp.float32)
    spread_level = 1.0
    direction = jax.random.normal(jax.random.fold_in(key, 12), (D,), jnp.float32)
    region_scale = jax.random.uniform(jax.random.fold_in(key, 13), (TOKENS // TOK_DEV,), jnp.float32, -1.2, 1.2)
    level = jnp.repeat(region_scale, TOK_DEV) * spread_level
    values = 0.8 * noise + level[:, None] * direction[None, :]
    return jnp.clip(values, -8.0, 8.0).astype(jnp.bfloat16)


def draw_head_bias(key, part):
    fast_count = HEADS // 2
    ranking = jax.random.permutation(jax.random.fold_in(key, 21), HEADS)
    is_fast = ranking < fast_count
    slow_value = -jnp.log(jnp.float32(TOKENS)) - 1.0 + jax.random.uniform(jax.random.fold_in(key, 22), (HEADS,), jnp.float32, -0.5, 0.5)
    fast_value = -jnp.log(jax.random.uniform(jax.random.fold_in(key, 23), (HEADS,), jnp.float32, 30.0, 100.0)) - 1.0
    return jnp.where(is_fast, fast_value, slow_value).astype(jnp.float32)


def levels(stream_key, extent, split, smallest, largest):
    gain, own = 1.0, jax.random.fold_in(stream_key, 6)
    for dim, shards_of in split:
        draws = jnp.exp(jax.random.uniform(jax.random.fold_in(own, dim), (shards_of,), jnp.float32, smallest / len(split), largest / len(split)))
        gain = gain * jnp.repeat(draws, extent[dim] // shards_of).reshape([-1 if axis == dim else 1 for axis in range(len(extent))])
    return gain


def centred(key, dims, deviation, bound, shards=(), kind=jnp.bfloat16):
    values = deviation * jax.random.normal(key, dims, jnp.float32)
    if shards:
        values = values * levels(key, dims, shards, -0.22, 0.18)
    return jnp.clip(values, -bound, bound).astype(kind)


def setup_inputs(seed: int = 0) -> dict:
    key_of = jax.random.split(jax.random.key(seed), 7)
    tokens = draw_tokens(jax.random.fold_in(key_of[6], 71), 0)
    w_query = centred(key_of[1], (D, HEADS * HEAD_DIM), D ** -0.5, 0.125, ((1, 8),))
    w_key = centred(key_of[2], (D, HEADS * HEAD_DIM), D ** -0.5, 0.125, ((1, 8),))
    w_value = centred(key_of[3], (D, HEADS * HEAD_DIM), D ** -0.5, 0.125, ((1, 8),))
    head_bias = draw_head_bias(jax.random.fold_in(key_of[6], 71), 0)
    w_out = centred(key_of[5], (HEADS * HEAD_DIM, D), (HEADS * HEAD_DIM) ** -0.5, 0.1875, ((0, 8),))
    return dict(tokens=tokens, w_query=w_query, w_key=w_key, w_value=w_value, head_bias=head_bias, w_out=w_out)


def reference(tokens, w_query, w_key, w_value, head_bias, w_out):
    query_all = jnp.dot(tokens, w_query, preferred_element_type=jnp.float32).astype(jnp.bfloat16)
    key_all = jnp.dot(tokens, w_key, preferred_element_type=jnp.float32).astype(jnp.bfloat16)
    value_all = jnp.dot(tokens, w_value, preferred_element_type=jnp.float32).astype(jnp.bfloat16)
    key_pos = jnp.arange(TOKENS, dtype=jnp.int32).reshape(N_SP, TOK_DEV)

    def by_head(head_index):
        first_col = (head_index * HEAD_DIM).astype(jnp.int32)
        query_head = lax.dynamic_slice_in_dim(query_all, first_col, HEAD_DIM, 1)
        key_head = lax.dynamic_slice_in_dim(key_all, first_col, HEAD_DIM, 1)
        value_head = lax.dynamic_slice_in_dim(value_all, first_col, HEAD_DIM, 1)
        value_segments = value_head.reshape(N_SP, TOK_DEV, HEAD_DIM).astype(jnp.float32)
        bias_value = head_bias[head_index]

        def by_block(block_index):
            first_row = (block_index * TOK_DEV).astype(jnp.int32)
            query_block = lax.dynamic_slice_in_dim(query_head, first_row, TOK_DEV, 0)
            query_pos = first_row + jnp.arange(TOK_DEV, dtype=jnp.int32)
            scores = jnp.dot(query_block, key_head.T, preferred_element_type=jnp.float32)
            scores = scores.reshape(TOK_DEV, N_SP, TOK_DEV) * (HEAD_DIM ** -0.5) + bias_value
            causal = key_pos[None] < query_pos[:, None, None]
            log_keep = jnp.where(causal, jax.nn.log_sigmoid(-scores), 0.0)
            tail = lax.cumsum(log_keep, axis=2, reverse=True) - log_keep
            weights = jnp.where(causal, jnp.exp(jax.nn.log_sigmoid(scores) + tail), 0.0).astype(jnp.bfloat16)
            segment_out = jnp.einsum('qst,std->qsd', weights.astype(jnp.float32), value_segments)
            segment_total = jnp.sum(log_keep, axis=2)
            later = lax.cumsum(segment_total, axis=1, reverse=True) - segment_total
            return jnp.sum(jnp.exp(later)[..., None] * segment_out, axis=1)

        return lax.map(by_block, jnp.arange(N_SP, dtype=jnp.int32)).reshape(TOKENS, HEAD_DIM)

    heads_out = lax.map(by_head, jnp.arange(HEADS, dtype=jnp.int32))
    attended = jnp.transpose(heads_out, (1, 0, 2)).reshape(TOKENS, HEADS * HEAD_DIM).astype(jnp.bfloat16)
    group_width = HEADS * HEAD_DIM // N_TP
    total = jnp.zeros((TOKENS, D), jnp.float32)
    for group_index in range(N_TP):
        lower = group_index * group_width
        partial_value = jnp.dot(attended[:, lower:lower + group_width], w_out[lower:lower + group_width, :],
                          preferred_element_type=jnp.float32).astype(jnp.bfloat16)
        partial_value = lax.optimization_barrier(partial_value)
        total = total + partial_value.astype(jnp.float32)
    return total.astype(jnp.bfloat16)
```

```python
import jax
import jax.numpy as jnp
from jax import lax
from jax.experimental import pallas as pl
from jax.experimental.pallas import tpu as pltpu
from jax.sharding import PartitionSpec as P

Z, Y, X, C = 8, 4, 4, 2
AXES = ("sp", "tp")
LANES = 128
TOK = 512
ROWS = 64
HEAD = 64
QROWS = 80
RUN = 16
CHUNK = 8 * RUN
DEPTH = 256
ZSEGS = 4


def moves(target):
    def index(z, y, x, c):
        return ((z * Y + y) * X + x) * C + c

    return [
        (index(z, y, x, c), index(*target(z, y, x, c)))
        for z in range(Z)
        for y in range(Y)
        for x in range(X)
        for c in range(C)
    ]


Z_UP = moves(lambda z, y, x, c: ((z + 1) % Z, y, x, c))
Z_DOWN = moves(lambda z, y, x, c: ((z - 1) % Z, y, x, c))
X_UP = moves(lambda z, y, x, c: (z, y, (x + 1) % X, c))
X_DOWN = moves(lambda z, y, x, c: (z, y, (x - 1) % X, c))
OTHER_CORE = moves(lambda z, y, x, c: (z, y, x, 1 - c))
KV_MOVE = [
    moves(lambda z, y, x, c, r=r: (z, 2 * c + (r ^ (y >> 1)), x, y & 1)) for r in range(2)
]
Q_MOVE = [
    moves(
        lambda z, y, x, c, r=r: (z, 2 * c + r, x, y)
        if y < 2
        else (Z - 1 - z, 2 * c + 1 - r, x, 3 - y)
    )
    for r in range(2)
]
Q_BACK = [[(d, s) for s, d in m] for m in Q_MOVE]


def send(a, move):
    return lax.ppermute(a, AXES, move)


def in_vmem():
    return pl.BlockSpec(memory_space=pltpu.VMEM)


def in_smem():
    return pl.BlockSpec(memory_space=pltpu.SMEM)


def project_body(pos, bias, *refs):
    tok, (wq, wk, wv) = refs[:10], refs[10:13]
    (q0, q1, kv0, kv1), (rows, q_t, kv) = refs[13:17], refs[17:]
    x, c, high = pos[1] // C, pos[1] % C, (pos[0] % Y) // 2
    for side in range(2):
        core = c if side == 0 else 1 - c
        for n, (far, first, count) in enumerate(((0, 0, 64), (3, 0, 64), (1, 0, 64), (2, 0, 32), (2, 32, 32))):
            start = (((x + far) % X) * C + core) * ROWS + first
            rows[pl.ds(pl.multiple_of(start, 32), count)] = tok[5 * side + n][...]
    full = rows[...]
    one = jnp.float32

    def product(w):
        return jnp.dot(full, w[...], preferred_element_type=one).astype(jnp.bfloat16)

    query = product(wq)
    q_t[...] = (query * jnp.bfloat16(HEAD**-0.5)).T
    key, value = product(wk), product(wv)
    place = lax.broadcasted_iota(jnp.int32, (CHUNK, CHUNK), 0)
    origin = lax.broadcasted_iota(jnp.int32, (CHUNK, CHUNK), 1)
    order = jnp.where((place % 8) * RUN + place // 8 == origin, 1.0, 0.0).astype(jnp.bfloat16)
    for k in range(2):
        cols = slice(k * HEAD, (k + 1) * HEAD)
        joined = jnp.concatenate([key[:, cols], value[:, cols]], axis=1)
        for s in range(0, TOK, CHUNK):
            kv[k, s : s + CHUNK] = jnp.dot(
                order, joined[s : s + CHUNK], preferred_element_type=one
            ).astype(jnp.bfloat16)
    row = lax.broadcasted_iota(jnp.int32, (16, TOK), 0)
    for r, (q_out, kv_out) in enumerate(((q0, kv0), (q1, kv1))):
        k = high if r == 0 else 1 - high
        kv_out[...] = kv[k]
        q_out[:HEAD] = q_t[pl.ds(pl.multiple_of(k * HEAD, HEAD), HEAD)]
        b = jnp.full((16, TOK), bias[k], one)
        b_hi = b.astype(jnp.bfloat16).astype(one)
        b_mid = (b - b_hi).astype(jnp.bfloat16).astype(one)
        b_lo = b - b_hi - b_mid
        parts = jnp.where(row == 0, b_hi, jnp.where(row == 1, b_mid, jnp.where(row == 2, b_lo, 0.0)))
        q_out[HEAD:] = parts.astype(jnp.bfloat16)


def project(pos, bias, pieces, weights):
    bf = jnp.bfloat16
    return pl.pallas_call(
        project_body,
        out_shape=(jax.ShapeDtypeStruct((QROWS, TOK), bf),) * 2
        + (jax.ShapeDtypeStruct((TOK, LANES), bf),) * 2,
        in_specs=[in_smem(), in_smem()] + [in_vmem()] * 13,
        out_specs=(in_vmem(),) * 4,
        scratch_shapes=[
            pltpu.VMEM((TOK, 2048), bf),
            pltpu.VMEM((2 * HEAD, TOK), bf),
            pltpu.VMEM((2, TOK, LANES), bf),
        ],
        cost_estimate=pl.CostEstimate(flops=2 * TOK * 2048 * 384, bytes_accessed=4 << 20, transcendentals=0),
        name="project",
    )(pos, bias, *pieces, *weights)


def chunk_weights(scores, ahead, carry, masked):
    sub = lax.broadcasted_iota(jnp.int32, (8, LANES), 0)
    if masked:
        gap = lax.broadcasted_iota(jnp.int32, (8, LANES), 1) + ahead - sub * RUN
    kept, out = None, [None] * RUN
    for v in range(RUN - 1, -1, -1):
        e = jnp.exp(jnp.minimum(scores[v * 8 : (v + 1) * 8], 87.0))
        keep = 1.0 / (1.0 + e)
        take = e * keep
        if masked:
            live = gap > v
            keep = jnp.where(live, keep, 1.0)
            take = jnp.where(live, take, 0.0)
        out[v] = take if kept is None else take * kept
        kept = keep if kept is None else kept * keep
    later = jnp.where(sub < 7, pltpu.roll(kept, 7, 0), 1.0)
    later = later * jnp.where(sub < 7, pltpu.roll(later, 7, 0), 1.0)
    later = later * jnp.where(sub < 6, pltpu.roll(later, 6, 0), 1.0)
    later = later * jnp.where(sub < 4, pltpu.roll(later, 4, 0), 1.0)
    total = jnp.broadcast_to((later * kept)[0:1], (8, LANES))
    scale = later * carry
    return jnp.concatenate([w * scale for w in out]).astype(jnp.bfloat16), carry * total


def segment(k_ref, v_ref, q_ref, w_ref, acc_ref, kept_ref, j, b, masked):
    carries = [jnp.ones((8, LANES), jnp.float32)] * (TOK // LANES)
    queries = q_ref[b]
    out = None
    for s in range(TOK - CHUNK, -1, -CHUNK):
        scores = jnp.dot(k_ref[j, s : s + CHUNK], queries, preferred_element_type=jnp.float32)
        for n in range(TOK // LANES):
            t = slice(n * LANES, (n + 1) * LANES)
            w_ref[s : s + CHUNK, t], carries[n] = chunk_weights(
                scores[:, t], n * LANES - s, carries[n], masked
            )
        if s % DEPTH == 0:
            part = jnp.dot(
                v_ref[j, :, s : s + DEPTH], w_ref[s : s + DEPTH], preferred_element_type=jnp.float32
            )
            out = part if out is None else out + part
    kept = kept_ref[b]
    acc_ref[b] = acc_ref[b] + kept[0:1] * out
    kept_ref[b] = kept * jnp.concatenate(carries, axis=1)


def attend_body(far, pos, q0, q1, mine, theirs, acc_ref, kept_ref, k_ref, v_ref, q_ref, w_ref):
    z, y, c = pos[0] // Y, pos[0] % Y, pos[1] % C
    first = ((z + far) % Z) * ZSEGS
    acc_ref[...] = jnp.zeros_like(acc_ref)
    kept_ref[...] = jnp.ones_like(kept_ref)
    lane = lax.broadcasted_iota(jnp.int32, (1, LANES), 1)
    is_key = jnp.where(lane < HEAD, 1.0, 0.0).astype(jnp.bfloat16)
    is_bias = jnp.where((lane >= HEAD) & (lane < HEAD + 3), 1.0, 0.0).astype(jnp.bfloat16)
    for n in range(4):
        kv = (mine if n < 2 else theirs)[n % 2]
        half = y % 2 if n % 2 == 0 else 1 - y % 2
        slot = 2 * half + (c if n < 2 else 1 - c)
        k_ref[slot] = kv * is_key + is_bias
        v_ref[slot] = kv.T[HEAD:]
    for b, q in enumerate((q0, q1)):
        q_ref[b, :QROWS] = q[...]
        q_ref[b, QROWS:] = jnp.zeros((LANES - QROWS, TOK), jnp.bfloat16)

    def step(n, _):
        b, j = n // ZSEGS, ZSEGS - 1 - n % ZSEGS
        low = b == y % 2
        block = jnp.where(low, 4 * z + c, 31 - 4 * z - c)
        ahead = block - (first + j)

        @pl.when(ahead > 0)
        def _():
            segment(k_ref, v_ref, q_ref, w_ref, acc_ref, kept_ref, j, b, False)

        @pl.when(ahead == 0)
        def _():
            segment(k_ref, v_ref, q_ref, w_ref, acc_ref, kept_ref, j, b, True)

        return 0

    lax.fori_loop(0, 2 * ZSEGS, step, 0)


def attend(far, pos, q0, q1, mine, theirs):
    bf = jnp.bfloat16

    def body(*refs):
        attend_body(far, *refs)

    return pl.pallas_call(
        body,
        out_shape=(
            jax.ShapeDtypeStruct((2, HEAD, TOK), jnp.float32),
            jax.ShapeDtypeStruct((2, 8, TOK), jnp.float32),
        ),
        in_specs=[in_smem()] + [in_vmem()] * 4,
        out_specs=(in_vmem(), in_vmem()),
        scratch_shapes=[
            pltpu.VMEM((ZSEGS, TOK, LANES), bf),
            pltpu.VMEM((ZSEGS, HEAD, TOK), bf),
            pltpu.VMEM((2, LANES, TOK), bf),
            pltpu.VMEM((TOK, TOK), bf),
        ],
        cost_estimate=pl.CostEstimate(flops=1 << 32, bytes_accessed=1 << 20, transcendentals=1 << 22),
        name=f"attend{far % Z}",
    )(pos, q0, q1, mine, theirs)


def merge_body(fars, pos, *refs):
    n = len(fars)
    accs, kepts, outs = refs[:n], refs[n : 2 * n], refs[2 * n :]
    z = pos[0] // Y
    groups = [(z + far) % Z for far in fars]
    for b in range(2):
        total = None
        for i in range(n):
            factor = jnp.ones((8, TOK), jnp.float32)
            for k in range(n):
                if k != i:
                    factor = factor * jnp.where(groups[k] > groups[i], kepts[k][b], 1.0)
            part = factor[0:1] * accs[i][b]
            total = part if total is None else total + part
        outs[b][...] = total.astype(jnp.bfloat16)


def merge(fars, pos, parts):
    def body(*refs):
        merge_body(fars, *refs)

    return pl.pallas_call(
        body,
        out_shape=(jax.ShapeDtypeStruct((HEAD, TOK), jnp.bfloat16),) * 2,
        in_specs=[in_smem()] + [in_vmem()] * (2 * len(fars)),
        out_specs=(in_vmem(),) * 2,
        name="merge",
    )(pos, *[a for a, _ in parts], *[k for _, k in parts])


def output_body(pos, att, *refs):
    ws, out = refs[:10], refs[10]
    x, c = pos[1] // C, pos[1] % C
    total = None
    for side in range(2):
        core = c if side == 0 else 1 - c
        for n, (far, first, count) in enumerate(((0, 0, 128), (3, 0, 128), (1, 0, 128), (2, 0, 64), (2, 64, 64))):
            rows = att[((x + far) % X) * C + core]
            part = jnp.dot(
                rows[:, first : first + count], ws[5 * side + n][...], preferred_element_type=jnp.float32
            )
            total = part if total is None else total + part
    out[...] = total.astype(jnp.bfloat16)


def output(pos, att, pieces):
    return pl.pallas_call(
        output_body,
        out_shape=jax.ShapeDtypeStruct((ROWS, 2048), jnp.bfloat16),
        in_specs=[in_smem()] + [in_vmem()] * 11,
        out_specs=in_vmem(),
        name="output",
    )(pos, att, *pieces)


def from_all_tp(a):
    half = a.shape[0] // 2
    down, up = send(a, X_UP), send(a, X_DOWN)
    across = [send(down[:half], X_UP), send(up[half:], X_DOWN)]
    mine = [a, down, up, *across]
    return mine + [send(p, OTHER_CORE) for p in mine]


def shards(tokens, w_query, w_key, w_value, head_bias, w_out):
    sp, tp = lax.axis_index("sp"), lax.axis_index("tp")
    pos = jnp.stack([sp, tp]).astype(jnp.int32)
    y = sp % Y
    pieces = from_all_tp(tokens)
    q0, q1, kv0, kv1 = project(pos, head_bias, pieces, (w_query, w_key, w_value))
    own = jnp.stack([send(kv0, KV_MOVE[0]), send(kv1, KV_MOVE[1])])
    q0, q1 = send(q0, Q_MOVE[0]), send(q1, Q_MOVE[1])
    w_pieces = from_all_tp(w_out)
    groups = [(0, own)]
    low = high = own
    for far in range(1, Z // 2):
        low, high = send(low, Z_UP), send(high, Z_DOWN)
        groups += [(-far, low), (far, high)]
    groups += [(Z // 2, jnp.stack([send(low[0], Z_UP), send(high[1], Z_DOWN)]))]
    fars = [far for far, _ in groups]
    parts = [attend(far, pos, q0, q1, kv, send(kv, OTHER_CORE)) for far, kv in groups]
    att0, att1 = merge(fars, pos, parts)
    att0, att1 = send(att0, Q_BACK[0]), send(att1, Q_BACK[1])
    att = jnp.where(y < 2, jnp.concatenate([att0, att1]), jnp.concatenate([att1, att0])).T
    att = lax.all_to_all(att.reshape(X * C, ROWS, 2 * HEAD), "tp", 0, 0, tiled=True)
    return output(pos, att, w_pieces)


def solution(mesh):
    placed = (
        P(("sp", "tp"), None),
        P(None, "tp"),
        P(None, "tp"),
        P(None, "tp"),
        P("tp"),
        P("tp", None),
    )
    return jax.shard_map(
        shards, mesh=mesh, in_specs=placed, out_specs=P(("sp", "tp"), None), check_vma=False
    )
```

```python
import jax
import jax.numpy as jnp
from jax import lax
from jax.experimental import pallas as pl
from jax.experimental.pallas import tpu as pltpu
from jax.sharding import PartitionSpec as P

Z, Y, X, C = 8, 4, 4, 2
AXES = ("sp", "tp")
LANES = 128
TOK = 512
ROWS = 64
HEAD = 64
QROWS = 80
RUN = 16
CHUNK = 8 * RUN
DEPTH = 256
ZSEGS = 4


def moves(target):
    def index(z, y, x, c):
        return ((z * Y + y) * X + x) * C + c

    return [
        (index(z, y, x, c), index(*target(z, y, x, c)))
        for z in range(Z)
        for y in range(Y)
        for x in range(X)
        for c in range(C)
    ]


Z_FIRST = moves(lambda z, y, x, c: ((z + 1 - 2 * c) % Z, y, x, c))
Z_SECOND = moves(lambda z, y, x, c: ((z - 1 + 2 * c) % Z, y, x, c))
X_FIRST = moves(lambda z, y, x, c: (z, y, (x + 1 - 2 * c) % X, c))
X_SECOND = moves(lambda z, y, x, c: (z, y, (x - 1 + 2 * c) % X, c))
OTHER_CORE = moves(lambda z, y, x, c: (z, y, x, 1 - c))
KV_MOVE = [
    moves(lambda z, y, x, c, r=r: (z, 2 * c + (r ^ (y >> 1)), x, y & 1)) for r in range(2)
]
Q_MOVE = [
    moves(
        lambda z, y, x, c, r=r: (z, 2 * c + r, x, y)
        if y < 2
        else (Z - 1 - z, 2 * c + 1 - r, x, 3 - y)
    )
    for r in range(2)
]
Q_BACK = [[(d, s) for s, d in m] for m in Q_MOVE]


def send(a, move):
    return lax.ppermute(a, AXES, move)


def in_vmem():
    return pl.BlockSpec(memory_space=pltpu.VMEM)


def in_smem():
    return pl.BlockSpec(memory_space=pltpu.SMEM)


def piece_origins(x, c):
    origins = []
    for core in (c, 1 - c):
        way = 1 - 2 * core
        origins += [((x - way * far + 2 * X) % X) * C + core for far in (0, 1, -1, 2)]
    return origins


def project_body(pos, bias, *refs):
    tok, (wq, wk, wv) = refs[:8], refs[8:11]
    (q0, q1, kv0, kv1), (rows, q_t, kv) = refs[11:15], refs[15:]
    x, c, high = pos[1] // C, pos[1] % C, (pos[0] % Y) // 2
    for n, origin in enumerate(piece_origins(x, c)):
        rows[pl.ds(pl.multiple_of(origin * ROWS, ROWS), ROWS)] = tok[n][...]
    full = rows[...]
    one, bf = jnp.float32, jnp.bfloat16

    def product(w):
        return jnp.dot(full, w[...], preferred_element_type=one).astype(bf)

    key, value, query = product(wk), product(wv), product(wq)
    q_t[...] = (query * bf(HEAD**-0.5)).T
    value_t = value.T
    place = lax.broadcasted_iota(jnp.int32, (CHUNK, CHUNK), 0)
    origin = lax.broadcasted_iota(jnp.int32, (CHUNK, CHUNK), 1)
    order = jnp.where((place % 8) * RUN + place // 8 == origin, 1.0, 0.0).astype(bf)
    order_t = jnp.where((origin % 8) * RUN + origin // 8 == place, 1.0, 0.0).astype(bf)
    keys = []
    for n in range(TOK // CHUNK):
        s = slice(n * CHUNK, (n + 1) * CHUNK)
        keys.append(jnp.dot(order, key[s], preferred_element_type=one).astype(bf))
        v_t = jnp.dot(value_t[:, s], order_t, preferred_element_type=one).astype(bf)
        for k in range(2):
            kv[k, 256 + n * HEAD : 256 + (n + 1) * HEAD] = v_t[k * HEAD : (k + 1) * HEAD]
    for n in range(2):
        s = slice(n * CHUNK, (n + 1) * CHUNK)
        for k in range(2):
            cols = slice(k * HEAD, (k + 1) * HEAD)
            kv[k, s] = jnp.concatenate([keys[n][:, cols], keys[n + 2][:, cols]], axis=1)
    row = lax.broadcasted_iota(jnp.int32, (16, TOK), 0)
    for r, (q_out, kv_out) in enumerate(((q0, kv0), (q1, kv1))):
        k = high if r == 0 else 1 - high
        kv_out[...] = kv[k]
        q_out[:HEAD] = q_t[pl.ds(pl.multiple_of(k * HEAD, HEAD), HEAD)]
        b = jnp.full((16, TOK), bias[k], one)
        b_hi = b.astype(bf).astype(one)
        b_mid = (b - b_hi).astype(bf).astype(one)
        b_lo = b - b_hi - b_mid
        parts = jnp.where(row == 0, b_hi, jnp.where(row == 1, b_mid, jnp.where(row == 2, b_lo, 0.0)))
        q_out[HEAD:] = parts.astype(bf)


def project(pos, bias, pieces, weights):
    bf = jnp.bfloat16
    return pl.pallas_call(
        project_body,
        out_shape=(jax.ShapeDtypeStruct((QROWS, TOK), bf),) * 2
        + (jax.ShapeDtypeStruct((TOK, LANES), bf),) * 2,
        in_specs=[in_smem(), in_smem()] + [in_vmem()] * 11,
        out_specs=(in_vmem(),) * 4,
        scratch_shapes=[
            pltpu.VMEM((TOK, 2048), bf),
            pltpu.VMEM((2 * HEAD, TOK), bf),
            pltpu.VMEM((2, TOK, LANES), bf),
        ],
        cost_estimate=pl.CostEstimate(flops=1 << 26, bytes_accessed=4 << 20, transcendentals=0),
        name="project",
    )(pos, bias, *pieces, *weights)


def chunk_weights(scores, ahead, carry, masked):
    sub = lax.broadcasted_iota(jnp.int32, (8, LANES), 0)
    if masked:
        gap = lax.broadcasted_iota(jnp.int32, (8, LANES), 1) + ahead - sub * RUN
    kept, out = None, [None] * RUN
    for v in range(RUN - 1, -1, -1):
        e = jnp.exp(jnp.minimum(scores[v * 8 : (v + 1) * 8], 87.0))
        keep = 1.0 / (1.0 + e)
        take = e * keep
        if masked:
            live = gap > v
            keep = jnp.where(live, keep, 1.0)
            take = jnp.where(live, take, 0.0)
        out[v] = take if kept is None else take * kept
        kept = keep if kept is None else kept * keep
    later = jnp.where(sub < 7, pltpu.roll(kept, 7, 0), 1.0)
    later = later * jnp.where(sub < 7, pltpu.roll(later, 7, 0), 1.0)
    later = later * jnp.where(sub < 6, pltpu.roll(later, 6, 0), 1.0)
    later = later * jnp.where(sub < 4, pltpu.roll(later, 4, 0), 1.0)
    total = jnp.broadcast_to((later * kept)[0:1], (8, LANES))
    scale = later * carry
    return jnp.concatenate([w * scale for w in out]).astype(jnp.bfloat16), carry * total


def segment(m_ref, q_ref, w_ref, acc_ref, kept_ref, place, g, b, masked):
    carries = [jnp.ones((8, LANES), jnp.float32)] * (TOK // LANES)
    lane = lax.broadcasted_iota(jnp.int32, (1, LANES), 1)
    ones = jnp.broadcast_to(jnp.where(lane < 3, 1.0, 0.0), (256, LANES)).astype(jnp.bfloat16)
    keys = jnp.concatenate([m_ref[place, :256], ones], axis=1)
    out = None
    for half in (1, 0):
        scores = jnp.dot(keys, q_ref[b, half], preferred_element_type=jnp.float32)
        for s in (CHUNK, 0):
            for n in range(TOK // LANES):
                t = slice(n * LANES, (n + 1) * LANES)
                w_ref[s : s + CHUNK, t], carries[n] = chunk_weights(
                    scores[s : s + CHUNK, t], n * LANES - s - 256 * half, carries[n], masked
                )
        first = 256 + 2 * HEAD * half
        values = jnp.concatenate(
            [m_ref[place, first : first + HEAD], m_ref[place, first + HEAD : first + 2 * HEAD]], axis=1
        )
        part = jnp.dot(values, w_ref[...], preferred_element_type=jnp.float32)
        out = part if out is None else out + part
    kept = kept_ref[g, b]
    acc_ref[g, b] = acc_ref[g, b] + kept[0:1] * out
    kept_ref[g, b] = kept * jnp.concatenate(carries, axis=1)


def group_of(z, c, far):
    return (z + (1 - 2 * c) * far + Z) % Z


def attend_body(fars, pos, q0, q1, *refs):
    count = len(fars)
    kvs, (acc_ref, kept_ref, m_ref, q_ref, w_ref) = refs[: 2 * count], refs[2 * count :]
    z, y, c = pos[0] // Y, pos[0] % Y, pos[1] % C
    acc_ref[...] = jnp.zeros_like(acc_ref)
    kept_ref[...] = jnp.ones_like(kept_ref)
    for g in range(count):
        for n in range(4):
            half = y % 2 if n % 2 == 0 else 1 - y % 2
            slot = 2 * half + (c if n < 2 else 1 - c)
            m_ref[ZSEGS * g + slot] = kvs[2 * g + n // 2][n % 2]
    q_ref[...] = jnp.zeros_like(q_ref)
    for b, q in enumerate((q0, q1)):
        for half in range(2):
            q_ref[b, half, HEAD * half : HEAD * (half + 1)] = q[:HEAD]
            q_ref[b, half, LANES : LANES + 16] = q[HEAD:]

    def step(n, _):
        g, b, j = n // (2 * ZSEGS), n // ZSEGS % 2, ZSEGS - 1 - n % ZSEGS
        far = jnp.where(g == 0, fars[0], fars[-1])
        block = jnp.where(b == y % 2, 4 * z + c, 31 - 4 * z - c)
        ahead = block - (group_of(z, c, far) * ZSEGS + j)
        args = (m_ref, q_ref, w_ref, acc_ref, kept_ref, ZSEGS * g + j, g, b)

        @pl.when(ahead > 0)
        def _():
            segment(*args, False)

        @pl.when(ahead == 0)
        def _():
            segment(*args, True)

        return 0

    lax.fori_loop(0, count * 2 * ZSEGS, step, 0)


def attend(fars, pos, q0, q1, kvs):
    bf = jnp.bfloat16
    count = len(fars)

    def body(*refs):
        attend_body(fars, *refs)

    return pl.pallas_call(
        body,
        out_shape=(
            jax.ShapeDtypeStruct((count, 2, HEAD, TOK), jnp.float32),
            jax.ShapeDtypeStruct((count, 2, 8, TOK), jnp.float32),
        ),
        in_specs=[in_smem()] + [in_vmem()] * (2 + 2 * count),
        out_specs=(in_vmem(), in_vmem()),
        scratch_shapes=[
            pltpu.VMEM((count * ZSEGS, TOK, LANES), bf),
            pltpu.VMEM((2, 2, 2 * LANES, TOK), bf),
            pltpu.VMEM((2 * CHUNK, TOK), bf),
        ],
        cost_estimate=pl.CostEstimate(flops=count << 31, bytes_accessed=1 << 20, transcendentals=1 << 22),
        name=f"attend{fars[-1]}",
    )(pos, q0, q1, *kvs)


def merge_body(fars, pos, *refs):
    n = len(fars)
    accs, kepts, outs = refs[:n], refs[n : 2 * n], refs[2 * n :]
    z, c = pos[0] // Y, pos[1] % C
    places = [(i, g, group_of(z, c, far)) for i in range(n) for g, far in enumerate(fars[i])]
    for b in range(2):
        total = None
        for i, g, group in places:
            factor = jnp.ones((8, TOK), jnp.float32)
            for k, h, other in places:
                if (k, h) != (i, g):
                    factor = factor * jnp.where(other > group, kepts[k][h, b], 1.0)
            part = factor[0:1] * accs[i][g, b]
            total = part if total is None else total + part
        outs[b][...] = total.astype(jnp.bfloat16)


def merge(fars, pos, parts):
    def body(*refs):
        merge_body(fars, *refs)

    return pl.pallas_call(
        body,
        out_shape=(jax.ShapeDtypeStruct((HEAD, TOK), jnp.bfloat16),) * 2,
        in_specs=[in_smem()] + [in_vmem()] * (2 * len(fars)),
        out_specs=(in_vmem(),) * 2,
        name="merge",
    )(pos, *[a for a, _ in parts], *[k for _, k in parts])


def output_body(pos, att, *refs):
    ws, out = refs[:8], refs[8]
    total = None
    for n, origin in enumerate(piece_origins(pos[1] // C, pos[1] % C)):
        part = jnp.dot(att[origin], ws[n][...], preferred_element_type=jnp.float32)
        total = part if total is None else total + part
    out[...] = total.astype(jnp.bfloat16)


def output(pos, att, pieces):
    return pl.pallas_call(
        output_body,
        out_shape=jax.ShapeDtypeStruct((ROWS, 2048), jnp.bfloat16),
        in_specs=[in_smem()] + [in_vmem()] * 9,
        out_specs=in_vmem(),
        name="output",
    )(pos, att, *pieces)


def after(a, *others):
    return lax.optimization_barrier((a, *others))[0]


def across_x(a):
    first, second = send(a, X_FIRST), send(a, X_SECOND)
    return [a, first, second, send(first, X_FIRST)]


def from_all_tp(mine):
    return mine + [send(p, OTHER_CORE) for p in mine]


def shards(tokens, w_query, w_key, w_value, head_bias, w_out):
    sp, tp = lax.axis_index("sp"), lax.axis_index("tp")
    pos = jnp.stack([sp, tp]).astype(jnp.int32)
    y = sp % Y
    mine = across_x(tokens)
    pieces = from_all_tp(mine)
    q0, q1, kv0, kv1 = project(pos, head_bias, pieces, (w_query, w_key, w_value))
    q0, q1 = send(q0, Q_MOVE[0]), send(q1, Q_MOVE[1])
    own = jnp.stack([send(kv0, KV_MOVE[0]), send(kv1, KV_MOVE[1])])
    fars = [(0,), (-1, 1), (-2, 2), (-3, 3), (4,)]
    steps = [(own,), (send(own, Z_FIRST), send(own, Z_SECOND))]
    theirs = [(send(own, OTHER_CORE),)]
    parts = []
    w_mine = across_x(after(w_out, own))
    w_pieces = []
    for n in range(len(fars)):
        if n + 1 < len(fars):
            ahead = after(steps[n + 1], *parts)
            theirs.append(tuple(send(a, OTHER_CORE) for a in reversed(ahead)))
            q0, q1, *_ = lax.optimization_barrier((q0, q1, *ahead))
            if n + 2 < len(fars) - 1:
                steps.append((send(ahead[0], Z_FIRST), send(ahead[1], Z_SECOND)))
            elif n + 2 == len(fars) - 1:
                steps.append((send(ahead[0], Z_FIRST),))
        else:
            q0, q1, *w_pieces = lax.optimization_barrier((q0, q1, *w_pieces))
        kvs = [a for pair in zip(steps[n], theirs[n]) for a in pair]
        parts.append(attend(fars[n], pos, q0, q1, kvs))
        if n == 1:
            w_pieces = from_all_tp([after(w, parts[n]) for w in w_mine])
    att0, att1 = merge(fars, pos, parts)
    att0, att1 = send(att0, Q_BACK[0]), send(att1, Q_BACK[1])
    att = jnp.where(y < 2, jnp.concatenate([att0, att1]), jnp.concatenate([att1, att0])).T
    att = lax.all_to_all(att.reshape(X * C, ROWS, 2 * HEAD), "tp", 0, 0, tiled=True)
    return output(pos, att, w_pieces)


def solution(mesh):
    placed = (
        P(("sp", "tp"), None),
        P(None, "tp"),
        P(None, "tp"),
        P(None, "tp"),
        P("tp"),
        P("tp", None),
    )
    return jax.shard_map(
        shards, mesh=mesh, in_specs=placed, out_specs=P(("sp", "tp"), None), check_vma=False
    )
```

```python
import jax
import jax.numpy as jnp
from jax import lax
from jax.experimental import pallas as pl
from jax.experimental.pallas import tpu as pltpu
from jax.sharding import PartitionSpec as P


Z, Y, X, C = 8, 4, 4, 2
AXES = ("sp", "tp")
LANES = 128
TOK = 512
ROWS = 64
HEAD = 64
QROWS = 80
RUN = 16
CHUNK = 8 * RUN
ZSEGS = 4


def moves(target):
    def index(z, y, x, c):
        return ((z * Y + y) * X + x) * C + c

    return [
        (index(z, y, x, c), index(*target(z, y, x, c)))
        for z in range(Z)
        for y in range(Y)
        for x in range(X)
        for c in range(C)
    ]


Z_FIRST = moves(lambda z, y, x, c: ((z + 1 - 2 * c) % Z, y, x, c))
Z_SECOND = moves(lambda z, y, x, c: ((z - 1 + 2 * c) % Z, y, x, c))
X_FIRST = moves(lambda z, y, x, c: (z, y, (x + 1 - 2 * c) % X, c))
X_SECOND = moves(lambda z, y, x, c: (z, y, (x - 1 + 2 * c) % X, c))
OTHER_CORE = moves(lambda z, y, x, c: (z, y, x, 1 - c))
KV_MOVE = [
    moves(lambda z, y, x, c, r=r: (z, 2 * c + (r ^ (y >> 1)), x, y & 1)) for r in range(2)
]
Q_MOVE = [
    moves(
        lambda z, y, x, c, r=r: (z, 2 * c + r, x, y)
        if y < 2
        else (Z - 1 - z, 2 * c + 1 - r, x, 3 - y)
    )
    for r in range(2)
]
Q_BACK = [[(d, s) for s, d in m] for m in Q_MOVE]


def send(a, move):
    return lax.ppermute(a, AXES, move)


def in_vmem():
    return pl.BlockSpec(memory_space=pltpu.VMEM)


def in_smem():
    return pl.BlockSpec(memory_space=pltpu.SMEM)


def piece_origins(x, c):
    origins = []
    for core in (c, 1 - c):
        way = 1 - 2 * core
        origins += [((x - way * far + 2 * X) % X) * C + core for far in (0, 1, -1, 2)]
    return origins


def project_body(pos, bias, *refs):
    tok, (wq, wk, wv) = refs[:8], refs[8:11]
    (q0, q1, kv0, kv1), (rows, q_t, kv) = refs[11:15], refs[15:]
    x, c, high = pos[1] // C, pos[1] % C, (pos[0] % Y) // 2
    for n, origin in enumerate(piece_origins(x, c)):
        rows[pl.ds(pl.multiple_of(origin * ROWS, ROWS), ROWS)] = tok[n][...]
    full = rows[...]
    one, bf = jnp.float32, jnp.bfloat16

    def product(w):
        return jnp.dot(full, w[...], preferred_element_type=one).astype(bf)

    key, value, query = product(wk), product(wv), product(wq)
    q_t[...] = (query * bf(HEAD**-0.5)).T
    value_t = value.T
    place = lax.broadcasted_iota(jnp.int32, (CHUNK, CHUNK), 0)
    origin = lax.broadcasted_iota(jnp.int32, (CHUNK, CHUNK), 1)
    order = jnp.where((place % 8) * RUN + place // 8 == origin, 1.0, 0.0).astype(bf)
    order_t = jnp.where((origin % 8) * RUN + origin // 8 == place, 1.0, 0.0).astype(bf)
    keys = []
    for n in range(TOK // CHUNK):
        s = slice(n * CHUNK, (n + 1) * CHUNK)
        keys.append(jnp.dot(order, key[s], preferred_element_type=one).astype(bf))
        v_t = jnp.dot(value_t[:, s], order_t, preferred_element_type=one).astype(bf)
        for k in range(2):
            kv[k, 256 + n * HEAD : 256 + (n + 1) * HEAD] = v_t[k * HEAD : (k + 1) * HEAD]
    for n in range(2):
        s = slice(n * CHUNK, (n + 1) * CHUNK)
        for k in range(2):
            cols = slice(k * HEAD, (k + 1) * HEAD)
            kv[k, s] = jnp.concatenate([keys[n][:, cols], keys[n + 2][:, cols]], axis=1)
    row = lax.broadcasted_iota(jnp.int32, (16, TOK), 0)
    for r, (q_out, kv_out) in enumerate(((q0, kv0), (q1, kv1))):
        k = high if r == 0 else 1 - high
        kv_out[...] = kv[k]
        q_out[:HEAD] = q_t[pl.ds(pl.multiple_of(k * HEAD, HEAD), HEAD)]
        b = jnp.full((16, TOK), bias[k], one)
        b_hi = b.astype(bf).astype(one)
        b_mid = (b - b_hi).astype(bf).astype(one)
        b_lo = b - b_hi - b_mid
        parts = jnp.where(row == 0, b_hi, jnp.where(row == 1, b_mid, jnp.where(row == 2, b_lo, 0.0)))
        q_out[HEAD:] = parts.astype(bf)


def project(pos, bias, pieces, weights):
    bf = jnp.bfloat16
    return pl.pallas_call(
        project_body,
        out_shape=(jax.ShapeDtypeStruct((QROWS, TOK), bf),) * 2
        + (jax.ShapeDtypeStruct((TOK, LANES), bf),) * 2,
        in_specs=[in_smem(), in_smem()] + [in_vmem()] * 11,
        out_specs=(in_vmem(),) * 4,
        scratch_shapes=[
            pltpu.VMEM((TOK, 2048), bf),
            pltpu.VMEM((2 * HEAD, TOK), bf),
            pltpu.VMEM((2, TOK, LANES), bf),
        ],
        cost_estimate=pl.CostEstimate(flops=1 << 26, bytes_accessed=4 << 20, transcendentals=0),
        name="project",
    )(pos, bias, *pieces, *weights)


def chunk_weights(scores, ahead, carry):
    masked = ahead is not None
    sub = lax.broadcasted_iota(jnp.int32, (8, LANES), 0)
    if masked:
        gap = lax.broadcasted_iota(jnp.int32, (8, LANES), 1) + ahead - sub * RUN
    kept, out = None, [None] * RUN
    for v in range(RUN - 1, -1, -1):
        e = jnp.exp(jnp.minimum(scores[v * 8 : (v + 1) * 8], 87.0))
        keep = 1.0 / (1.0 + e)
        take = e * keep
        if masked:
            live = gap > v
            keep = jnp.where(live, keep, 1.0)
            take = jnp.where(live, take, 0.0)
        out[v] = take if kept is None else take * kept
        kept = keep if kept is None else kept * keep
    later = jnp.where(sub < 7, pltpu.roll(kept, 7, 0), 1.0)
    later = later * jnp.where(sub < 7, pltpu.roll(later, 7, 0), 1.0)
    later = later * jnp.where(sub < 6, pltpu.roll(later, 6, 0), 1.0)
    later = later * jnp.where(sub < 4, pltpu.roll(later, 4, 0), 1.0)
    total = jnp.broadcast_to((later * kept)[0:1], (8, LANES))
    scale = later * carry
    return jnp.concatenate([w * scale for w in out]).astype(jnp.bfloat16), carry * total


def segments(m_ref, q_ref, w_ref, acc_ref, kept_ref, places, g, b, ahead):
    carries = [jnp.ones((8, LANES), jnp.float32)] * (TOK // LANES)
    lane = lax.broadcasted_iota(jnp.int32, (1, LANES), 1)
    ones = jnp.broadcast_to(jnp.where(lane < 3, 1.0, 0.0), (256, LANES)).astype(jnp.bfloat16)
    out = None
    for i, place in enumerate(places):
        keys = jnp.concatenate([m_ref[place, :256], ones], axis=1)
        for half in (1, 0):
            scores = jnp.dot(keys, q_ref[b, half], preferred_element_type=jnp.float32)
            w = w_ref.at[2 * i + half]
            for s in (CHUNK, 0):
                for n in range(TOK // LANES):
                    t = slice(n * LANES, (n + 1) * LANES)
                    start = n * LANES - s - 256 * half
                    w[s : s + CHUNK, t], carries[n] = chunk_weights(
                        scores[s : s + CHUNK, t],
                        None if ahead is None else start + TOK * ahead,
                        carries[n],
                    )
            first = 256 + 2 * HEAD * half
            values = jnp.concatenate(
                [m_ref[place, first : first + HEAD], m_ref[place, first + HEAD : first + 2 * HEAD]],
                axis=1,
            )
            part = jnp.dot(values, w[...], preferred_element_type=jnp.float32)
            out = part if out is None else out + part
    kept = kept_ref[g, b]
    acc_ref[g, b] = acc_ref[g, b] + kept[0:1] * out
    kept_ref[g, b] = kept * jnp.concatenate(carries, axis=1)


def group_of(z, c, far):
    return (z + (1 - 2 * c) * far + Z) % Z


def attend_body(fars, pos, q0, q1, *refs):
    count = len(fars)
    kvs, (acc_ref, kept_ref, m_ref, q_ref, w_ref) = refs[: 2 * count], refs[2 * count :]
    z, y, c = pos[0] // Y, pos[0] % Y, pos[1] % C
    acc_ref[...] = jnp.zeros_like(acc_ref)
    kept_ref[...] = jnp.ones_like(kept_ref)
    for g in range(count):
        for n in range(4):
            half = y % 2 if n % 2 == 0 else 1 - y % 2
            slot = 2 * half + (c if n < 2 else 1 - c)
            m_ref[ZSEGS * g + slot] = kvs[2 * g + n // 2][n % 2]
    q_ref[...] = jnp.zeros_like(q_ref)
    for b, q in enumerate((q0, q1)):
        for half in range(2):
            q_ref[b, half, HEAD * half : HEAD * (half + 1)] = q[:HEAD]
            q_ref[b, half, LANES : LANES + 16] = q[HEAD:]

    def side(n, _):
        g, b = n // 2, n % 2
        far = jnp.where(g == 0, fars[0], fars[-1])
        block = jnp.where(b == y % 2, 4 * z + c, 31 - 4 * z - c)
        ahead = block - group_of(z, c, far) * ZSEGS
        refs = (m_ref, q_ref, w_ref, acc_ref, kept_ref)

        @pl.when(ahead >= ZSEGS)
        def _():
            def pair(i, _):
                j = ZSEGS * g + ZSEGS - 1 - 2 * i
                segments(*refs, (j, j - 1), g, b, None)
                return 0

            lax.fori_loop(0, ZSEGS // 2, pair, 0)

        if fars[-1] % 2 or fars == (0,):

            @pl.when((ahead >= 0) & (ahead < ZSEGS))
            def _():
                def single(i, _):
                    segments(*refs, (ZSEGS * g + ahead - i,), g, b, i)
                    return 0

                lax.fori_loop(0, ahead + 1, single, 0)

        return 0

    lax.fori_loop(0, count * 2, side, 0)


def attend(fars, pos, q0, q1, kvs):
    bf = jnp.bfloat16
    count = len(fars)

    def body(*refs):
        attend_body(fars, *refs)

    return pl.pallas_call(
        body,
        out_shape=(
            jax.ShapeDtypeStruct((count, 2, HEAD, TOK), jnp.float32),
            jax.ShapeDtypeStruct((count, 2, 8, TOK), jnp.float32),
        ),
        in_specs=[in_smem()] + [in_vmem()] * (2 + 2 * count),
        out_specs=(in_vmem(), in_vmem()),
        scratch_shapes=[
            pltpu.VMEM((count * ZSEGS, TOK, LANES), bf),
            pltpu.VMEM((2, 2, 2 * LANES, TOK), bf),
            pltpu.VMEM((4, 2 * CHUNK, TOK), bf),
        ],
        cost_estimate=pl.CostEstimate(flops=count << 31, bytes_accessed=1 << 20, transcendentals=1 << 22),
    )(pos, q0, q1, *kvs)


def merge_body(fars, pos, *refs):
    n = len(fars)
    accs, kepts, outs = refs[:n], refs[n : 2 * n], refs[2 * n :]
    z, c = pos[0] // Y, pos[1] % C
    places = [(i, g, group_of(z, c, far)) for i in range(n) for g, far in enumerate(fars[i])]
    for b in range(2):
        total = None
        for i, g, group in places:
            factor = jnp.ones((8, TOK), jnp.float32)
            for k, h, other in places:
                if (k, h) != (i, g):
                    factor = factor * jnp.where(other > group, kepts[k][h, b], 1.0)
            part = factor[0:1] * accs[i][g, b]
            total = part if total is None else total + part
        outs[b][...] = total.astype(jnp.bfloat16)


def merge(fars, pos, parts):
    def body(*refs):
        merge_body(fars, *refs)

    return pl.pallas_call(
        body,
        out_shape=(jax.ShapeDtypeStruct((HEAD, TOK), jnp.bfloat16),) * 2,
        in_specs=[in_smem()] + [in_vmem()] * (2 * len(fars)),
        out_specs=(in_vmem(),) * 2,
        name="merge",
    )(pos, *[a for a, _ in parts], *[k for _, k in parts])


def output_body(pos, att, *refs):
    ws, out = refs[:8], refs[8]
    total = None
    for n, origin in enumerate(piece_origins(pos[1] // C, pos[1] % C)):
        part = jnp.dot(att[origin], ws[n][...], preferred_element_type=jnp.float32)
        total = part if total is None else total + part
    out[...] = total.astype(jnp.bfloat16)


def output(pos, att, pieces):
    return pl.pallas_call(
        output_body,
        out_shape=jax.ShapeDtypeStruct((ROWS, 2048), jnp.bfloat16),
        in_specs=[in_smem()] + [in_vmem()] * 9,
        out_specs=in_vmem(),
        name="output",
    )(pos, att, *pieces)


def after(a, *others):
    return lax.optimization_barrier((a, *others))[0]


def across_x(a):
    first, second = send(a, X_FIRST), send(a, X_SECOND)
    return [a, first, second, send(first, X_FIRST)]


def from_all_tp(mine):
    return mine + [send(p, OTHER_CORE) for p in mine]


def shards(tokens, w_query, w_key, w_value, head_bias, w_out):
    sp, tp = lax.axis_index("sp"), lax.axis_index("tp")
    pos = jnp.stack([sp, tp]).astype(jnp.int32)
    y = sp % Y
    mine = across_x(tokens)
    pieces = from_all_tp(mine)
    q0, q1, kv0, kv1 = project(pos, head_bias, pieces, (w_query, w_key, w_value))
    q0, q1 = send(q0, Q_MOVE[0]), send(q1, Q_MOVE[1])
    own = jnp.stack([send(kv0, KV_MOVE[0]), send(kv1, KV_MOVE[1])])
    fars = [(0,), (-1, 1), (-2, 2), (-3, 3), (4,)]
    steps = [(own,), (send(own, Z_FIRST), send(own, Z_SECOND))]
    theirs = [(send(own, OTHER_CORE),)]
    parts = []
    w_mine = across_x(after(w_out, own))
    w_pieces = []
    for n in range(len(fars)):
        if n + 1 < len(fars):
            ahead = after(steps[n + 1], *parts)
            theirs.append(tuple(send(a, OTHER_CORE) for a in reversed(ahead)))
            q0, q1, *_ = lax.optimization_barrier((q0, q1, *ahead))
            if n + 2 < len(fars) - 1:
                steps.append((send(ahead[0], Z_FIRST), send(ahead[1], Z_SECOND)))
            elif n + 2 == len(fars) - 1:
                steps.append((send(ahead[0], Z_FIRST),))
        else:
            q0, q1, *w_pieces = lax.optimization_barrier((q0, q1, *w_pieces))
        kvs = [a for pair in zip(steps[n], theirs[n]) for a in pair]
        parts.append(attend(fars[n], pos, q0, q1, kvs))
        if n == 1:
            w_pieces = from_all_tp([after(w, parts[n]) for w in w_mine])
    att0, att1 = merge(fars, pos, parts)
    att0, att1 = send(att0, Q_BACK[0]), send(att1, Q_BACK[1])
    att = jnp.where(y < 2, jnp.concatenate([att0, att1]), jnp.concatenate([att1, att0])).T
    att = lax.all_to_all(att.reshape(X * C, ROWS, 2 * HEAD), "tp", 0, 0, tiled=True)
    return output(pos, att, w_pieces)


def solution(mesh):
    placed = (
        P(("sp", "tp"), None),
        P(None, "tp"),
        P(None, "tp"),
        P(None, "tp"),
        P("tp"),
        P("tp", None),
    )

    return jax.shard_map(
        shards, mesh=mesh, in_specs=placed, out_specs=P(("sp", "tp"), None), check_vma=False
    )
```

```python
import jax
import jax.numpy as jnp
from jax import lax
from jax.experimental import pallas as pl
from jax.experimental.pallas import tpu as pltpu
from jax.sharding import PartitionSpec as P


Z, Y, X, C = 8, 4, 4, 2
AXES = ("sp", "tp")
LANES = 128
TOK = 512
ROWS = 64
HEAD = 64
QROWS = 80
RUN = 16
CHUNK = 8 * RUN
ZSEGS = 4


def moves(target):
    def index(z, y, x, c):
        return ((z * Y + y) * X + x) * C + c

    return [
        (index(z, y, x, c), index(*target(z, y, x, c)))
        for z in range(Z)
        for y in range(Y)
        for x in range(X)
        for c in range(C)
    ]


Z_FIRST = moves(lambda z, y, x, c: ((z + 1 - 2 * c) % Z, y, x, c))
Z_SECOND = moves(lambda z, y, x, c: ((z - 1 + 2 * c) % Z, y, x, c))
X_FIRST = moves(lambda z, y, x, c: (z, y, (x + 1 - 2 * c) % X, c))
X_SECOND = moves(lambda z, y, x, c: (z, y, (x - 1 + 2 * c) % X, c))
OTHER_CORE = moves(lambda z, y, x, c: (z, y, x, 1 - c))
KV_MOVE = [
    moves(lambda z, y, x, c, r=r: (z, 2 * c + (r ^ (y >> 1)), x, y & 1)) for r in range(2)
]
Q_MOVE = [
    moves(
        lambda z, y, x, c, r=r: (z, 2 * c + r, x, y)
        if y < 2
        else (Z - 1 - z, 2 * c + 1 - r, x, 3 - y)
    )
    for r in range(2)
]
Q_BACK = [[(d, s) for s, d in m] for m in Q_MOVE]


def send(a, move):
    return lax.ppermute(a, AXES, move)


def in_vmem():
    return pl.BlockSpec(memory_space=pltpu.VMEM)


def in_smem():
    return pl.BlockSpec(memory_space=pltpu.SMEM)


def piece_origins(x, c):
    origins = []
    for core in (c, 1 - c):
        way = 1 - 2 * core
        origins += [((x - way * far + 2 * X) % X) * C + core for far in (0, 1, -1, 2)]
    return origins


def project_body(pos, bias, *refs):
    tok, (wq, wk, wv) = refs[:8], refs[8:11]
    (q0, q1, kv0, kv1), (rows, q_t, kv) = refs[11:15], refs[15:]
    x, c, high = pos[1] // C, pos[1] % C, (pos[0] % Y) // 2
    for n, origin in enumerate(piece_origins(x, c)):
        rows[pl.ds(pl.multiple_of(origin * ROWS, ROWS), ROWS)] = tok[n][...]
    full = rows[...]
    one, bf = jnp.float32, jnp.bfloat16

    def product(w):
        return jnp.dot(full, w[...], preferred_element_type=one).astype(bf)

    key, value, query = product(wk), product(wv), product(wq)
    q_t[...] = (query * bf(HEAD**-0.5)).T
    value_t = value.T
    place = lax.broadcasted_iota(jnp.int32, (CHUNK, CHUNK), 0)
    origin = lax.broadcasted_iota(jnp.int32, (CHUNK, CHUNK), 1)
    order = jnp.where((place % 8) * RUN + place // 8 == origin, 1.0, 0.0).astype(bf)
    order_t = jnp.where((origin % 8) * RUN + origin // 8 == place, 1.0, 0.0).astype(bf)
    keys = []
    for n in range(TOK // CHUNK):
        s = slice(n * CHUNK, (n + 1) * CHUNK)
        keys.append(jnp.dot(order, key[s], preferred_element_type=one).astype(bf))
        v_t = jnp.dot(value_t[:, s], order_t, preferred_element_type=one).astype(bf)
        for k in range(2):
            kv[k, 256 + n * HEAD : 256 + (n + 1) * HEAD] = v_t[k * HEAD : (k + 1) * HEAD]
    for n in range(2):
        s = slice(n * CHUNK, (n + 1) * CHUNK)
        for k in range(2):
            cols = slice(k * HEAD, (k + 1) * HEAD)
            kv[k, s] = jnp.concatenate([keys[n][:, cols], keys[n + 2][:, cols]], axis=1)
    row = lax.broadcasted_iota(jnp.int32, (16, TOK), 0)
    for r, (q_out, kv_out) in enumerate(((q0, kv0), (q1, kv1))):
        k = high if r == 0 else 1 - high
        kv_out[...] = kv[k]
        q_out[:HEAD] = q_t[pl.ds(pl.multiple_of(k * HEAD, HEAD), HEAD)]
        b = jnp.full((16, TOK), bias[k], one)
        b_hi = b.astype(bf).astype(one)
        b_mid = (b - b_hi).astype(bf).astype(one)
        b_lo = b - b_hi - b_mid
        parts = jnp.where(row == 0, b_hi, jnp.where(row == 1, b_mid, jnp.where(row == 2, b_lo, 0.0)))
        q_out[HEAD:] = parts.astype(bf)


def project(pos, bias, pieces, weights):
    bf = jnp.bfloat16
    return pl.pallas_call(
        project_body,
        out_shape=(jax.ShapeDtypeStruct((QROWS, TOK), bf),) * 2
        + (jax.ShapeDtypeStruct((TOK, LANES), bf),) * 2,
        in_specs=[in_smem(), in_smem()] + [in_vmem()] * 11,
        out_specs=(in_vmem(),) * 4,
        scratch_shapes=[
            pltpu.VMEM((TOK, 2048), bf),
            pltpu.VMEM((2 * HEAD, TOK), bf),
            pltpu.VMEM((2, TOK, LANES), bf),
        ],
        cost_estimate=pl.CostEstimate(flops=1 << 26, bytes_accessed=4 << 20, transcendentals=0),
        name="project",
    )(pos, bias, *pieces, *weights)


def chunk_weights(scores, ahead, carry):
    masked = ahead is not None
    sub = lax.broadcasted_iota(jnp.int32, (8, LANES), 0)
    if masked:
        gap = lax.broadcasted_iota(jnp.int32, (8, LANES), 1) + ahead - sub * RUN
    kept, out = None, [None] * RUN
    for v in range(RUN - 1, -1, -1):
        e = jnp.exp(jnp.minimum(scores[v * 8 : (v + 1) * 8], 87.0))
        keep = 1.0 / (1.0 + e)
        take = e * keep
        if masked:
            live = gap > v
            keep = jnp.where(live, keep, 1.0)
            take = jnp.where(live, take, 0.0)
        out[v] = take if kept is None else take * kept
        kept = keep if kept is None else kept * keep
    later = jnp.where(sub < 7, pltpu.roll(kept, 7, 0), 1.0)
    later = later * jnp.where(sub < 7, pltpu.roll(later, 7, 0), 1.0)
    later = later * jnp.where(sub < 6, pltpu.roll(later, 6, 0), 1.0)
    later = later * jnp.where(sub < 4, pltpu.roll(later, 4, 0), 1.0)
    total = jnp.broadcast_to((later * kept)[0:1], (8, LANES))
    scale = later * carry
    return jnp.concatenate([w * scale for w in out]).astype(jnp.bfloat16), carry * total


def segments(m_ref, q_ref, w_ref, acc_ref, kept_ref, places, g, b, ahead):
    carries = [jnp.ones((8, LANES), jnp.float32)] * (TOK // LANES)
    lane = lax.broadcasted_iota(jnp.int32, (1, LANES), 1)
    ones = jnp.broadcast_to(jnp.where(lane < 3, 1.0, 0.0), (256, LANES)).astype(jnp.bfloat16)
    out = None
    stages = [(i, half) for i in range(len(places)) for half in (1, 0)]

    def scores_of(i, half):
        keys = jnp.concatenate([m_ref[places[i], :256], ones], axis=1)
        return jnp.dot(keys, q_ref[b, half], preferred_element_type=jnp.float32)

    def product(i, half):
        first = 256 + 2 * HEAD * half
        values = [m_ref[places[i], first + n * HEAD : first + (n + 1) * HEAD] for n in range(2)]
        return jnp.dot(
            jnp.concatenate(values, axis=1), w_ref[2 * i + half], preferred_element_type=jnp.float32
        )

    following = scores_of(*stages[0])
    for k, (i, half) in enumerate(stages):
        scores = following
        if k + 1 < len(stages):
            following = scores_of(*stages[k + 1])
        if k:
            part = product(*stages[k - 1])
            out = part if out is None else out + part
        for s in (CHUNK, 0):
            for n in range(TOK // LANES):
                t = slice(n * LANES, (n + 1) * LANES)
                start = n * LANES - s - 256 * half
                w_ref[2 * i + half, s : s + CHUNK, t], carries[n] = chunk_weights(
                    scores[s : s + CHUNK, t],
                    None if ahead is None else start + TOK * ahead,
                    carries[n],
                )
    out = out + product(*stages[-1])
    kept = kept_ref[g, b]
    acc_ref[g, b] = acc_ref[g, b] + kept[0:1] * out
    kept_ref[g, b] = kept * jnp.concatenate(carries, axis=1)


def group_of(z, c, far):
    return (z + (1 - 2 * c) * far + Z) % Z


def attend_body(fars, pos, q0, q1, *refs):
    count = len(fars)
    kvs, (acc_ref, kept_ref, m_ref, q_ref, w_ref) = refs[: 2 * count], refs[2 * count :]
    z, y, c = pos[0] // Y, pos[0] % Y, pos[1] % C
    acc_ref[...] = jnp.zeros_like(acc_ref)
    kept_ref[...] = jnp.ones_like(kept_ref)
    for g in range(count):
        for n in range(4):
            half = y % 2 if n % 2 == 0 else 1 - y % 2
            slot = 2 * half + (c if n < 2 else 1 - c)
            m_ref[ZSEGS * g + slot] = kvs[2 * g + n // 2][n % 2]
    q_ref[...] = jnp.zeros_like(q_ref)
    for b, q in enumerate((q0, q1)):
        for half in range(2):
            q_ref[b, half, HEAD * half : HEAD * (half + 1)] = q[:HEAD]
            q_ref[b, half, LANES : LANES + 16] = q[HEAD:]

    def side(n, _):
        g, b = n // 2, n % 2
        far = jnp.where(g == 0, fars[0], fars[-1])
        block = jnp.where(b == y % 2, 4 * z + c, 31 - 4 * z - c)
        ahead = block - group_of(z, c, far) * ZSEGS
        refs = (m_ref, q_ref, w_ref, acc_ref, kept_ref)

        @pl.when(ahead >= ZSEGS)
        def _():
            def pair(i, _):
                j = ZSEGS * g + ZSEGS - 1 - 2 * i
                segments(*refs, (j, j - 1), g, b, None)
                return 0

            lax.fori_loop(0, ZSEGS // 2, pair, 0)

        if fars[-1] % 2 or fars == (0,):

            @pl.when((ahead >= 0) & (ahead < ZSEGS))
            def _():
                def single(i, _):
                    segments(*refs, (ZSEGS * g + ahead - i,), g, b, i)
                    return 0

                lax.fori_loop(0, ahead + 1, single, 0)

        return 0

    lax.fori_loop(0, count * 2, side, 0)


def attend(fars, pos, q0, q1, kvs):
    bf = jnp.bfloat16
    count = len(fars)

    def body(*refs):
        attend_body(fars, *refs)

    return pl.pallas_call(
        body,
        out_shape=(
            jax.ShapeDtypeStruct((count, 2, HEAD, TOK), jnp.float32),
            jax.ShapeDtypeStruct((count, 2, 8, TOK), jnp.float32),
        ),
        in_specs=[in_smem()] + [in_vmem()] * (2 + 2 * count),
        out_specs=(in_vmem(), in_vmem()),
        scratch_shapes=[
            pltpu.VMEM((count * ZSEGS, TOK, LANES), bf),
            pltpu.VMEM((2, 2, 2 * LANES, TOK), bf),
            pltpu.VMEM((4, 2 * CHUNK, TOK), bf),
        ],
        cost_estimate=pl.CostEstimate(flops=count << 31, bytes_accessed=1 << 20, transcendentals=1 << 22),
    )(pos, q0, q1, *kvs)


def merge_body(fars, pos, *refs):
    n = len(fars)
    accs, kepts, outs = refs[:n], refs[n : 2 * n], refs[2 * n :]
    z, c = pos[0] // Y, pos[1] % C
    places = [(i, g, group_of(z, c, far)) for i in range(n) for g, far in enumerate(fars[i])]
    for b in range(2):
        total = None
        for i, g, group in places:
            factor = jnp.ones((8, TOK), jnp.float32)
            for k, h, other in places:
                if (k, h) != (i, g):
                    factor = factor * jnp.where(other > group, kepts[k][h, b], 1.0)
            part = factor[0:1] * accs[i][g, b]
            total = part if total is None else total + part
        outs[b][...] = total.astype(jnp.bfloat16)


def merge(fars, pos, parts):
    def body(*refs):
        merge_body(fars, *refs)

    return pl.pallas_call(
        body,
        out_shape=(jax.ShapeDtypeStruct((HEAD, TOK), jnp.bfloat16),) * 2,
        in_specs=[in_smem()] + [in_vmem()] * (2 * len(fars)),
        out_specs=(in_vmem(),) * 2,
        name="merge",
    )(pos, *[a for a, _ in parts], *[k for _, k in parts])


def output_body(pos, att, *refs):
    ws, out = refs[:8], refs[8]
    total = None
    for n, origin in enumerate(piece_origins(pos[1] // C, pos[1] % C)):
        part = jnp.dot(att[origin], ws[n][...], preferred_element_type=jnp.float32)
        total = part if total is None else total + part
    out[...] = total.astype(jnp.bfloat16)


def output(pos, att, pieces):
    return pl.pallas_call(
        output_body,
        out_shape=jax.ShapeDtypeStruct((ROWS, 2048), jnp.bfloat16),
        in_specs=[in_smem()] + [in_vmem()] * 9,
        out_specs=in_vmem(),
        name="output",
    )(pos, att, *pieces)


def after(a, *others):
    return lax.optimization_barrier((a, *others))[0]


def across_x(a, *before):
    first, second = send(a, X_FIRST), send(a, X_SECOND)
    return [a, first, second, send(after(first, *before), X_FIRST)]


def from_all_tp(mine):
    return mine + [send(p, OTHER_CORE) for p in mine]


def shards(tokens, w_query, w_key, w_value, head_bias, w_out):
    sp, tp = lax.axis_index("sp"), lax.axis_index("tp")
    pos = jnp.stack([sp, tp]).astype(jnp.int32)
    y = sp % Y
    mine = across_x(tokens, pos)
    pieces = from_all_tp(mine)
    q0, q1, kv0, kv1 = project(pos, head_bias, pieces, (w_query, w_key, w_value))
    q0, q1 = send(q0, Q_MOVE[0]), send(q1, Q_MOVE[1])
    own = jnp.stack([send(kv0, KV_MOVE[0]), send(kv1, KV_MOVE[1])])
    fars = [(0,), (-1, 1), (-2, 2), (-3, 3), (4,)]
    steps = [(own,), (send(own, Z_FIRST), send(own, Z_SECOND))]
    theirs = [(send(own, OTHER_CORE),)]
    parts = []
    w_mine = across_x(after(w_out, own))
    w_pieces = []
    for n in range(len(fars)):
        if n + 1 < len(fars):
            ahead = after(steps[n + 1], *parts)
            theirs.append(tuple(send(a, OTHER_CORE) for a in reversed(ahead)))
            q0, q1, *_ = lax.optimization_barrier((q0, q1, *ahead))
            if n + 2 < len(fars) - 1:
                steps.append((send(ahead[0], Z_FIRST), send(ahead[1], Z_SECOND)))
            elif n + 2 == len(fars) - 1:
                steps.append((send(ahead[0], Z_FIRST),))
        else:
            q0, q1, *w_pieces = lax.optimization_barrier((q0, q1, *w_pieces))
        kvs = [a for pair in zip(steps[n], theirs[n]) for a in pair]
        parts.append(attend(fars[n], pos, q0, q1, kvs))
        if n == 1:
            w_pieces = from_all_tp([after(w, parts[n]) for w in w_mine])
    att0, att1 = merge(fars, pos, parts)
    att0, att1 = send(att0, Q_BACK[0]), send(att1, Q_BACK[1])
    att = jnp.where(y < 2, jnp.concatenate([att0, att1]), jnp.concatenate([att1, att0])).T
    att = lax.all_to_all(att.reshape(X * C, ROWS, 2 * HEAD), "tp", 0, 0, tiled=True)
    return output(pos, att, w_pieces)


def solution(mesh):
    placed = (
        P(("sp", "tp"), None),
        P(None, "tp"),
        P(None, "tp"),
        P(None, "tp"),
        P("tp"),
        P("tp", None),
    )

    return jax.shard_map(
        shards, mesh=mesh, in_specs=placed, out_specs=P(("sp", "tp"), None), check_vma=False
    )
```

```python
import jax
import jax.numpy as jnp
from jax import lax
from jax.experimental import pallas as pl
from jax.experimental.pallas import tpu as pltpu
from jax.sharding import PartitionSpec as P


Z, Y, X, C = 8, 4, 4, 2
AXES = ("sp", "tp")
LANES = 128
TOK = 512
ROWS = 64
HEAD = 64
QROWS = 80
RUN = 16
CHUNK = 8 * RUN
ZSEGS = 4


def moves(target):
    def index(z, y, x, c):
        return ((z * Y + y) * X + x) * C + c

    return [
        (index(z, y, x, c), index(*target(z, y, x, c)))
        for z in range(Z)
        for y in range(Y)
        for x in range(X)
        for c in range(C)
    ]


Z_FIRST = moves(lambda z, y, x, c: ((z + 1 - 2 * c) % Z, y, x, c))
Z_SECOND = moves(lambda z, y, x, c: ((z - 1 + 2 * c) % Z, y, x, c))
X_FIRST = moves(lambda z, y, x, c: (z, y, (x + 1 - 2 * c) % X, c))
X_SECOND = moves(lambda z, y, x, c: (z, y, (x - 1 + 2 * c) % X, c))
OTHER_CORE = moves(lambda z, y, x, c: (z, y, x, 1 - c))
KV_MOVE = [
    moves(lambda z, y, x, c, r=r: (z, 2 * c + (r ^ (y >> 1)), x, y & 1)) for r in range(2)
]
Q_MOVE = [
    moves(
        lambda z, y, x, c, r=r: (z, 2 * c + r, x, y)
        if y < 2
        else (Z - 1 - z, 2 * c + 1 - r, x, 3 - y)
    )
    for r in range(2)
]
Q_BACK = [[(d, s) for s, d in m] for m in Q_MOVE]


def send(a, move):
    return lax.ppermute(a, AXES, move)


def in_vmem():
    return pl.BlockSpec(memory_space=pltpu.VMEM)


def in_smem():
    return pl.BlockSpec(memory_space=pltpu.SMEM)


def piece_origins(x, c):
    origins = []
    for core in (c, 1 - c):
        way = 1 - 2 * core
        origins += [((x - way * far + 2 * X) % X) * C + core for far in (0, 1, -1, 2)]
    return origins


def project_body(pos, bias, *refs):
    tok, (wq, wk, wv) = refs[:8], refs[8:11]
    (q0, q1, kv0, kv1), (rows, q_t, kv) = refs[11:15], refs[15:]
    x, c, high = pos[1] // C, pos[1] % C, (pos[0] % Y) // 2
    for n, origin in enumerate(piece_origins(x, c)):
        rows[pl.ds(pl.multiple_of(origin * ROWS, ROWS), ROWS)] = tok[n][...]
    full = rows[...]
    one, bf = jnp.float32, jnp.bfloat16

    def product(w):
        return jnp.dot(full, w[...], preferred_element_type=one).astype(bf)

    key, value, query = product(wk), product(wv), product(wq)
    q_t[...] = (query * bf(HEAD**-0.5)).T
    value_t = value.T
    place = lax.broadcasted_iota(jnp.int32, (CHUNK, CHUNK), 0)
    origin = lax.broadcasted_iota(jnp.int32, (CHUNK, CHUNK), 1)
    order = jnp.where((place % 8) * RUN + place // 8 == origin, 1.0, 0.0).astype(bf)
    order_t = jnp.where((origin % 8) * RUN + origin // 8 == place, 1.0, 0.0).astype(bf)
    keys = []
    for n in range(TOK // CHUNK):
        s = slice(n * CHUNK, (n + 1) * CHUNK)
        keys.append(jnp.dot(order, key[s], preferred_element_type=one).astype(bf))
        v_t = jnp.dot(value_t[:, s], order_t, preferred_element_type=one).astype(bf)
        for k in range(2):
            kv[k, 256 + n * HEAD : 256 + (n + 1) * HEAD] = v_t[k * HEAD : (k + 1) * HEAD]
    for n in range(2):
        s = slice(n * CHUNK, (n + 1) * CHUNK)
        for k in range(2):
            cols = slice(k * HEAD, (k + 1) * HEAD)
            kv[k, s] = jnp.concatenate([keys[n][:, cols], keys[n + 2][:, cols]], axis=1)
    row = lax.broadcasted_iota(jnp.int32, (16, TOK), 0)
    for r, (q_out, kv_out) in enumerate(((q0, kv0), (q1, kv1))):
        k = high if r == 0 else 1 - high
        kv_out[...] = kv[k]
        q_out[:HEAD] = q_t[pl.ds(pl.multiple_of(k * HEAD, HEAD), HEAD)]
        b = jnp.full((16, TOK), bias[k], one)
        b_hi = b.astype(bf).astype(one)
        b_mid = (b - b_hi).astype(bf).astype(one)
        b_lo = b - b_hi - b_mid
        parts = jnp.where(row == 0, b_hi, jnp.where(row == 1, b_mid, jnp.where(row == 2, b_lo, 0.0)))
        q_out[HEAD:] = parts.astype(bf)


def project(pos, bias, pieces, weights):
    bf = jnp.bfloat16
    return pl.pallas_call(
        project_body,
        out_shape=(jax.ShapeDtypeStruct((QROWS, TOK), bf),) * 2
        + (jax.ShapeDtypeStruct((TOK, LANES), bf),) * 2,
        in_specs=[in_smem(), in_smem()] + [in_vmem()] * 11,
        out_specs=(in_vmem(),) * 4,
        scratch_shapes=[
            pltpu.VMEM((TOK, 2048), bf),
            pltpu.VMEM((2 * HEAD, TOK), bf),
            pltpu.VMEM((2, TOK, LANES), bf),
        ],
        cost_estimate=pl.CostEstimate(flops=1 << 26, bytes_accessed=4 << 20, transcendentals=0),
        name="project",
    )(pos, bias, *pieces, *weights)


def chunk_weights(scores, ahead, carry):
    masked = ahead is not None
    sub = lax.broadcasted_iota(jnp.int32, (8, LANES), 0)
    if masked:
        gap = lax.broadcasted_iota(jnp.int32, (8, LANES), 1) + ahead - sub * RUN
    kept, out = None, [None] * RUN
    for v in range(RUN - 1, -1, -1):
        e = jnp.exp(jnp.minimum(scores[v * 8 : (v + 1) * 8], 87.0))
        keep = 1.0 / (1.0 + e)
        take = e * keep
        if masked:
            live = gap > v
            keep = jnp.where(live, keep, 1.0)
            take = jnp.where(live, take, 0.0)
        out[v] = take if kept is None else take * kept
        kept = keep if kept is None else kept * keep
    later = jnp.where(sub < 7, pltpu.roll(kept, 7, 0), 1.0)
    later = later * jnp.where(sub < 7, pltpu.roll(later, 7, 0), 1.0)
    later = later * jnp.where(sub < 6, pltpu.roll(later, 6, 0), 1.0)
    later = later * jnp.where(sub < 4, pltpu.roll(later, 4, 0), 1.0)
    total = jnp.broadcast_to((later * kept)[0:1], (8, LANES))
    scale = later * carry
    return jnp.concatenate([w * scale for w in out]).astype(jnp.bfloat16), carry * total


def segments(m_ref, q_ref, w_ref, acc_ref, kept_ref, places, g, b, ahead):
    carries = [jnp.ones((8, LANES), jnp.float32)] * (TOK // LANES)
    lane = lax.broadcasted_iota(jnp.int32, (1, LANES), 1)
    ones = jnp.broadcast_to(jnp.where(lane < 3, 1.0, 0.0), (256, LANES)).astype(jnp.bfloat16)
    out = None
    stages = [(i, half) for i in range(len(places)) for half in (1, 0)]

    def scores_of(i, half):
        keys = jnp.concatenate([m_ref[places[i], :256], ones], axis=1)
        return jnp.dot(keys, q_ref[b, half], preferred_element_type=jnp.float32)

    def product(i, half):
        first = 256 + 2 * HEAD * half
        values = [m_ref[places[i], first + n * HEAD : first + (n + 1) * HEAD] for n in range(2)]
        return jnp.dot(
            jnp.concatenate(values, axis=1), w_ref[2 * i + half], preferred_element_type=jnp.float32
        )

    following = scores_of(*stages[0])
    for k, (i, half) in enumerate(stages):
        scores = following
        if k + 1 < len(stages):
            following = scores_of(*stages[k + 1])
        if k:
            part = product(*stages[k - 1])
            out = part if out is None else out + part
        for s in (CHUNK, 0):
            for n in range(TOK // LANES):
                t = slice(n * LANES, (n + 1) * LANES)
                start = n * LANES - s - 256 * half
                w_ref[2 * i + half, s : s + CHUNK, t], carries[n] = chunk_weights(
                    scores[s : s + CHUNK, t],
                    None if ahead is None else start + TOK * ahead,
                    carries[n],
                )
    out = out + product(*stages[-1])
    kept = kept_ref[g, b]
    acc_ref[g, b] = acc_ref[g, b] + kept[0:1] * out
    kept_ref[g, b] = kept * jnp.concatenate(carries, axis=1)


def group_of(z, c, far):
    return (z + (1 - 2 * c) * far + Z) % Z


def attend_body(fars, pos, q0, q1, *refs):
    count = len(fars)
    kvs, (acc_ref, kept_ref, m_ref, q_ref, w_ref) = refs[: 2 * count], refs[2 * count :]
    z, y, c = pos[0] // Y, pos[0] % Y, pos[1] % C
    acc_ref[...] = jnp.zeros_like(acc_ref)
    kept_ref[...] = jnp.ones_like(kept_ref)
    for g in range(count):
        for n in range(4):
            half = y % 2 if n % 2 == 0 else 1 - y % 2
            slot = 2 * half + (c if n < 2 else 1 - c)
            m_ref[ZSEGS * g + slot] = kvs[2 * g + n // 2][n % 2]
    q_ref[...] = jnp.zeros_like(q_ref)
    for b, q in enumerate((q0, q1)):
        for half in range(2):
            q_ref[b, half, HEAD * half : HEAD * (half + 1)] = q[:HEAD]
            q_ref[b, half, LANES : LANES + 16] = q[HEAD:]

    def side(n, _):
        g, b = n // 2, n % 2
        far = jnp.where(g == 0, fars[0], fars[-1])
        block = jnp.where(b == y % 2, 4 * z + c, 31 - 4 * z - c)
        ahead = block - group_of(z, c, far) * ZSEGS
        refs = (m_ref, q_ref, w_ref, acc_ref, kept_ref)

        @pl.when(ahead >= ZSEGS)
        def _():
            def pair(i, _):
                j = ZSEGS * g + ZSEGS - 1 - 2 * i
                segments(*refs, (j, j - 1), g, b, None)
                return 0

            lax.fori_loop(0, ZSEGS // 2, pair, 0)

        if fars[-1] % 2 or fars == (0,):

            @pl.when((ahead >= 0) & (ahead < ZSEGS))
            def _():
                def single(i, _):
                    segments(*refs, (ZSEGS * g + ahead - i,), g, b, i)
                    return 0

                lax.fori_loop(0, ahead + 1, single, 0)

        return 0

    lax.fori_loop(0, count * 2, side, 0)


def attend(fars, pos, q0, q1, kvs):
    bf = jnp.bfloat16
    count = len(fars)

    def body(*refs):
        attend_body(fars, *refs)

    return pl.pallas_call(
        body,
        out_shape=(
            jax.ShapeDtypeStruct((count, 2, HEAD, TOK), jnp.float32),
            jax.ShapeDtypeStruct((count, 2, 8, TOK), jnp.float32),
        ),
        in_specs=[in_smem()] + [in_vmem()] * (2 + 2 * count),
        out_specs=(in_vmem(), in_vmem()),
        scratch_shapes=[
            pltpu.VMEM((count * ZSEGS, TOK, LANES), bf),
            pltpu.VMEM((2, 2, 2 * LANES, TOK), bf),
            pltpu.VMEM((4, 2 * CHUNK, TOK), bf),
        ],
        cost_estimate=pl.CostEstimate(flops=count << 31, bytes_accessed=1 << 20, transcendentals=1 << 22),
    )(pos, q0, q1, *kvs)


def merge_body(fars, pos, *refs):
    n = len(fars)
    accs, kepts, outs = refs[:n], refs[n : 2 * n], refs[2 * n :]
    z, c = pos[0] // Y, pos[1] % C
    places = [(i, g, group_of(z, c, far)) for i in range(n) for g, far in enumerate(fars[i])]
    for b in range(2):
        total = None
        for i, g, group in places:
            factor = jnp.ones((8, TOK), jnp.float32)
            for k, h, other in places:
                if (k, h) != (i, g):
                    factor = factor * jnp.where(other > group, kepts[k][h, b], 1.0)
            part = factor[0:1] * accs[i][g, b]
            total = part if total is None else total + part
        outs[b][...] = total.astype(jnp.bfloat16)


def merge(fars, pos, parts):
    def body(*refs):
        merge_body(fars, *refs)

    return pl.pallas_call(
        body,
        out_shape=(jax.ShapeDtypeStruct((HEAD, TOK), jnp.bfloat16),) * 2,
        in_specs=[in_smem()] + [in_vmem()] * (2 * len(fars)),
        out_specs=(in_vmem(),) * 2,
        name="merge",
    )(pos, *[a for a, _ in parts], *[k for _, k in parts])


def output_body(pos, att, *refs):
    ws, out = refs[:8], refs[8]
    total = None
    for n, origin in enumerate(piece_origins(pos[1] // C, pos[1] % C)):
        part = jnp.dot(att[origin], ws[n][...], preferred_element_type=jnp.float32)
        total = part if total is None else total + part
    out[...] = total.astype(jnp.bfloat16)


def output(pos, att, pieces):
    return pl.pallas_call(
        output_body,
        out_shape=jax.ShapeDtypeStruct((ROWS, 2048), jnp.bfloat16),
        in_specs=[in_smem()] + [in_vmem()] * 9,
        out_specs=in_vmem(),
        name="output",
    )(pos, att, *pieces)


def after(a, *others):
    return lax.optimization_barrier((a, *others))[0]


def across_x(a, *before):
    first, second = send(a, X_FIRST), send(a, X_SECOND)
    return [a, first, second, send(after(first, *before), X_FIRST)]


def from_all_tp(mine):
    return mine + [send(p, OTHER_CORE) for p in mine]


def shards(tokens, w_query, w_key, w_value, head_bias, w_out):
    sp, tp = lax.axis_index("sp"), lax.axis_index("tp")
    pos = jnp.stack([sp, tp]).astype(jnp.int32)
    y = sp % Y
    mine = across_x(tokens, pos)
    pieces = from_all_tp(mine)
    q0, q1, kv0, kv1 = project(pos, head_bias, pieces, (w_query, w_key, w_value))
    q0, q1 = send(q0, Q_MOVE[0]), send(q1, Q_MOVE[1])
    own = jnp.stack([send(kv0, KV_MOVE[0]), send(kv1, KV_MOVE[1])])
    fars = [(0,), (-1, 1), (-2, 2), (-3, 3), (4,)]
    steps = [(own,), (send(own, Z_FIRST), send(own, Z_SECOND))]
    theirs = [(send(own, OTHER_CORE),)]
    parts = []
    w_pieces = []
    for n in range(len(fars)):
        if n + 1 < len(fars):
            ahead = after(steps[n + 1], *parts)
            theirs.append(tuple(send(a, OTHER_CORE) for a in reversed(ahead)))
            q0, q1, *_ = lax.optimization_barrier((q0, q1, *ahead))
            if n + 2 < len(fars) - 1:
                steps.append((send(ahead[0], Z_FIRST), send(ahead[1], Z_SECOND)))
            elif n + 2 == len(fars) - 1:
                steps.append((send(ahead[0], Z_FIRST),))
        else:
            q0, q1, *w_pieces = lax.optimization_barrier((q0, q1, *w_pieces))
        kvs = [a for pair in zip(steps[n], theirs[n]) for a in pair]
        parts.append(attend(fars[n], pos, q0, q1, kvs))
        if n == 0:
            w_mine = across_x(after(w_out, parts[0]))
        if n == 2:
            w_pieces = from_all_tp([after(w, parts[n]) for w in w_mine])
    att0, att1 = merge(fars, pos, parts)
    att0, att1 = send(att0, Q_BACK[0]), send(att1, Q_BACK[1])
    att = jnp.where(y < 2, jnp.concatenate([att0, att1]), jnp.concatenate([att1, att0])).T
    att = lax.all_to_all(att.reshape(X * C, ROWS, 2 * HEAD), "tp", 0, 0, tiled=True)
    return output(pos, att, w_pieces)


def solution(mesh):
    placed = (
        P(("sp", "tp"), None),
        P(None, "tp"),
        P(None, "tp"),
        P(None, "tp"),
        P("tp"),
        P("tp", None),
    )

    return jax.shard_map(
        shards, mesh=mesh, in_specs=placed, out_specs=P(("sp", "tp"), None), check_vma=False
    )
```
